32 devices in a mesh: sp: 8 (over z, y), tp: 4 (over x, core).
Axes of the slice: x: 2, y: 2, z: 4, core: 2. Of those that a mesh axis runs over, the one named last changes fastest.
Arguments:
- tokens: bfloat16 [6144, 2048], P('sp'), may hold values from -6 to 6
- input_gain: bfloat16 [2048], replicated, may hold values from 0.099609375 to 1.8984375
- gate_weight: bfloat16 [2048, 2048], P('sp', 'tp'), may hold values from -0.125 to 0.125
- value_weight: bfloat16 [2048, 2048], P('sp', 'tp'), may hold values from -0.125 to 0.125
- inflow_weight: bfloat16 [2048, 4, 128], P('sp', 'tp'), may hold values from -0.125 to 0.125
- readout_weight: bfloat16 [2048, 4, 128], P('sp', 'tp'), may hold values from -0.125 to 0.125
- step_weight: bfloat16 [2048, 2, 32], P('sp', None, 'tp'), may hold values from -0.125 to 0.125
- conv_values: bfloat16 [5, 2048], P(None, 'tp'), may hold values from -2.5 to 2.5
- conv_inflow: bfloat16 [5, 4, 128], P(None, 'tp'), may hold values from -2.5 to 2.5
- conv_readout: bfloat16 [5, 4, 128], P(None, 'tp'), may hold values from -2.5 to 2.5
- log_rate: float32 [2, 6144, 32], P(None, 'sp', 'tp'), may hold values from -20 to 0
- group_gain: bfloat16 [2048], P('tp'), may hold values from 0.099609375 to 1.8984375
- query_weight: bfloat16 [2048, 2048], P('sp', 'tp'), may hold values from -8 to 8
- key_weight: bfloat16 [2048, 512], P('sp', 'tp'), may hold values from -8 to 8
- vector_weight: bfloat16 [2048, 512], P('sp', 'tp'), may hold values from -0.125 to 0.125
- sink_logit: float32 [32], P('tp'), may hold values from 3 to 7
- state_out: bfloat16 [2048, 2048], P('tp', 'sp'), may hold values from -0.125 to 0.125
- window_out: bfloat16 [2048, 2048], P('tp', 'sp'), may hold values from -1 to 1
Outputs:
- mixed: bfloat16 [6144, 2048], P('sp', 'tp')
- log_total: float32 [6144, 32], P('sp', 'tp')
The draws below stay inside these ranges and needn't reach their ends.
All inputs are finite; a program needn't handle non-finite values.
Results may differ from the reference program's by a relative error of at most 0.015.
The reference program's roundings to bfloat16 on the way count: a program that leaves them out, or rounds other values in their place, can miss the bound.
Values may be sent and summed in bfloat16 or wider, within the bound.
A program may use at most 128 MiB of HBM per device.

```python
import jax
import jax.numpy as jnp
from jax import lax

D = 2048
SSD_HEADS = 32
HEAD_DIM = 64
GROUPS = 4
STATE = 128
CONV = 5
SSD_BLOCK = 128
ATT_HEADS = 32
KV_HEADS = 8
WINDOW = 128
QBLOCK = 256
GRID_W = 64
TOK_DEV = 768
TOKENS = 6144
INNER = 2048
ATT_WIDTH = 2048
KV_WIDTH = 512
N_TP = 4


def shared_query(key):
    base = jax.random.normal(jax.random.fold_in(key, 11), (D, ATT_HEADS, HEAD_DIM), jnp.float32)
    return base * D ** (-0.5)


def draw_query_weight(key, part):
    base = jnp.clip(shared_query(key), -8.0, 8.0)
    return base.reshape(D, ATT_HEADS * HEAD_DIM).astype(jnp.bfloat16)


def draw_key_weight(key, part):
    fresh = jax.random.normal(jax.random.fold_in(key, 12), (D, KV_HEADS, HEAD_DIM), jnp.float32) * D ** (-0.5)
    return jnp.clip(fresh, -8.0, 8.0).reshape(D, KV_HEADS * HEAD_DIM).astype(jnp.bfloat16)


def draw_log_rate(key, part):
    tensor_shape = (2, TOKENS, SSD_HEADS)
    per_group = SSD_HEADS // GROUPS
    chance = 0.5
    ranking = jax.random.permutation(jax.random.fold_in(key, 20), GROUPS)
    quick_group = jax.random.uniform(jax.random.fold_in(key, 21), (GROUPS,), jnp.float32) < chance
    quick_group = jnp.where(ranking == 0, True, jnp.where(ranking == 1, False, quick_group))
    quick_level = jnp.broadcast_to(jnp.repeat(quick_group, per_group)[None, None, :], (2, 1, SSD_HEADS))
    fast_level = jnp.log(jax.random.uniform(jax.random.fold_in(key, 22), (2, 1, SSD_HEADS), jnp.float32, 1.0 / 100.0, 1.0 / 40.0))
    slow_level = jnp.log(jax.random.uniform(jax.random.fold_in(key, 23), (2, 1, SSD_HEADS), jnp.float32, 0.3, 1.5) / TOKENS)
    depth_level = jnp.where(quick_level, fast_level, slow_level)
    blocks = TOKENS // TOK_DEV
    offset_shift = jax.random.uniform(jax.random.fold_in(key, 24), (2, blocks, 1, SSD_HEADS), jnp.float32, -0.7, 0.7)
    offset_shift = jnp.broadcast_to(offset_shift, (2, blocks, TOK_DEV, SSD_HEADS)).reshape(tensor_shape)
    coarse_rough = jax.random.uniform(jax.random.fold_in(key, 25), tensor_shape, jnp.float32, -0.3, 0.3)
    label_marks = jax.random.randint(jax.random.fold_in(key, 26), (1, TOKENS, 1), 0, TOKENS) < 6
    spike_amount = jnp.log(jax.random.uniform(jax.random.fold_in(key, 27), tensor_shape, jnp.float32, 0.3, 1.0))
    final_result = jnp.where(label_marks & jnp.logical_not(quick_level), spike_amount, depth_level + offset_shift + coarse_rough)
    return jnp.clip(final_result, -20.0, 0.0)


def steps_of(own_key, dims, split, least, top_value):
    def one(axis_at, shards_of):
        draws = jax.random.uniform(jax.random.fold_in(jax.random.fold_in(own_key, 6), axis_at), (shards_of,), jnp.float32, least / len(split), top_value / len(split))
        return jnp.repeat(jnp.exp(draws), dims[axis_at] // shards_of).reshape((-1,) + (1,) * (len(dims) - axis_at - 1))

    factor_of = one(*split[0])
    for cut in split[1:]:
        factor_of = factor_of * one(*cut)
    return factor_of


def centred(key, shape, scale, bound, shards=(), kind=jnp.bfloat16):
    factor_of = steps_of(key, shape, shards, -0.22, 0.18) if shards else 1.0
    array = jax.random.normal(key, shape, jnp.float32) * scale * factor_of
    return jnp.minimum(jnp.maximum(array, -bound), bound).astype(kind)


def setup_inputs(seed: int = 0) -> dict:
    key_list = jax.random.split(jax.random.key(seed), 19)
    tokens = centred(key_list[0], (TOKENS, D), 1.0, 6.0, ((0, 8),))
    input_gain = jnp.clip(1.0 + 0.18 * jax.random.normal(key_list[1], (D,), jnp.float32), 0.099609375, 1.8984375).astype(jnp.bfloat16)
    gate_weight = centred(key_list[2], (D, INNER), D ** -0.5, 0.125, ((0, 8), (1, 4)))
    value_weight = centred(key_list[3], (D, INNER), D ** -0.5, 0.125, ((0, 8), (1, 4)))
    inflow_weight = centred(key_list[4], (D, GROUPS, STATE), D ** -0.5, 0.125, ((0, 8), (1, 4)))
    readout_weight = centred(key_list[5], (D, GROUPS, STATE), D ** -0.5, 0.125, ((0, 8), (1, 4)))
    step_weight = centred(key_list[6], (D, 2, SSD_HEADS), D ** -0.5, 0.125, ((0, 8), (2, 4)))
    conv_values = centred(key_list[7], (CONV, INNER), CONV ** -0.5, 2.5, ((1, 4),))
    conv_inflow = centred(key_list[8], (CONV, GROUPS, STATE), CONV ** -0.5, 2.5, ((1, 4),))
    conv_readout = centred(key_list[9], (CONV, GROUPS, STATE), CONV ** -0.5, 2.5, ((1, 4),))
    log_rate = draw_log_rate(jax.random.fold_in(key_list[18], 71), 0)
    group_gain = jnp.clip(1.0 + 0.18 * jax.random.normal(key_list[11], (INNER,), jnp.float32), 0.099609375, 1.8984375).astype(jnp.bfloat16)
    query_weight = draw_query_weight(jax.random.fold_in(key_list[18], 71), 0)
    key_weight = draw_key_weight(jax.random.fold_in(key_list[18], 71), 0)
    vector_weight = centred(key_list[14], (D, KV_WIDTH), D ** -0.5, 0.125, ((0, 8), (1, 4)))
    sink_logit = jnp.clip(3.0 + 4.0 * jax.random.uniform(key_list[15], (ATT_HEADS,), jnp.float32) ** steps_of(key_list[15], (ATT_HEADS,), ((0, 4),), -0.2, 0.2), 3.0, 7.0)
    state_out = centred(key_list[16], (INNER, D), INNER ** -0.5, 0.125, ((0, 4), (1, 8)))
    window_out = centred(key_list[17], (ATT_WIDTH, D), (ATT_WIDTH // 64) ** -0.5, 1.0, ((0, 4), (1, 8)))
    return {"tokens": tokens, "input_gain": input_gain, "gate_weight": gate_weight, "value_weight": value_weight, "inflow_weight": inflow_weight, "readout_weight": readout_weight, "step_weight": step_weight, "conv_values": conv_values, "conv_inflow": conv_inflow, "conv_readout": conv_readout, "log_rate": log_rate, "group_gain": group_gain, "query_weight": query_weight, "key_weight": key_weight, "vector_weight": vector_weight, "sink_logit": sink_logit, "state_out": state_out, "window_out": window_out}


EPS = 1e-06
ROPE_BASE = 10000.0
HIGH = lax.Precision.HIGH

def rope_pairs(part, angle):
    half = part.shape[-1] // 2
    cosine = jnp.cos(angle)[:, None, :]
    sine = jnp.sin(angle)[:, None, :]
    first = part[..., :half]
    second = part[..., half:]
    return jnp.concatenate([first * cosine - second * sine, second * cosine + first * sine], axis=-1)

def axial_rope(heads, positions):
    width = heads.shape[-1]
    quarter = width // 4
    freqs = ROPE_BASE ** (-jnp.arange(quarter).astype(jnp.float32) / quarter)
    row_angle = (positions // GRID_W).astype(jnp.float32)[:, None] * freqs
    col_angle = (positions % GRID_W).astype(jnp.float32)[:, None] * freqs
    half = width // 2
    wide = heads.astype(jnp.float32)
    turned = jnp.concatenate([rope_pairs(wide[..., :half], row_angle), rope_pairs(wide[..., half:], col_angle)], axis=-1)
    return turned.astype(jnp.bfloat16)

def block_ssd(state, inputs):
    xdt, decay, inflow, readout = inputs
    length = decay.shape[0]
    heads = xdt.shape[1]
    groups = inflow.shape[1]
    repeat = heads // groups
    cum = jnp.cumsum(decay, axis=0)
    seg = cum[:, None, :] - cum[None, :, :]
    lower = jnp.arange(length)[:, None] >= jnp.arange(length)[None, :]
    weight = jnp.exp(jnp.where(lower[:, :, None], seg, -jnp.inf))
    intersection = jnp.einsum('lgn,sgn->lsg', readout.astype(jnp.bfloat16), inflow.astype(jnp.bfloat16), preferred_element_type=jnp.float32)
    intersection = jnp.repeat(intersection, repeat, axis=2)
    final_result = jnp.einsum('lsh,shp->lhp', intersection * weight, xdt, precision=HIGH)
    read_heads = jnp.repeat(readout, repeat, axis=1)
    final_result = final_result + jnp.exp(cum)[:, :, None] * jnp.einsum('lhn,hpn->lhp', read_heads, state, precision=HIGH)
    write_heads = jnp.repeat(inflow, repeat, axis=1)
    to_end = jnp.exp(cum[-1][None, :] - cum)
    fresh = jnp.einsum('shp,shn->hpn', xdt * to_end[:, :, None], write_heads, precision=HIGH)
    return (jnp.exp(cum[-1])[:, None, None] * state + fresh, final_result)

def run_blocks(xdt, decay, inflow, readout):
    count = decay.shape[0]
    blocks = count // SSD_BLOCK
    start_state = jnp.zeros((SSD_HEADS, HEAD_DIM, STATE), jnp.float32)
    shaped = (xdt.reshape(blocks, SSD_BLOCK, SSD_HEADS, HEAD_DIM), decay.reshape(blocks, SSD_BLOCK, SSD_HEADS), inflow.reshape(blocks, SSD_BLOCK, GROUPS, STATE), readout.reshape(blocks, SSD_BLOCK, GROUPS, STATE))
    final_state, final_result = lax.scan(block_ssd, start_state, shaped)
    return final_result.reshape(count, SSD_HEADS, HEAD_DIM)

def reference(tokens, input_gain, gate_weight, value_weight, inflow_weight, readout_weight, step_weight, conv_values, conv_inflow, conv_readout, log_rate, group_gain, query_weight, key_weight, vector_weight, sink_logit, state_out, window_out):
    count = tokens.shape[0]
    wide = tokens.astype(jnp.float32)
    normed = (wide * lax.rsqrt(lax.optimization_barrier(jnp.mean(wide * wide, axis=1, keepdims=True)) + EPS) * input_gain.astype(jnp.float32)).astype(jnp.bfloat16)

    def project(weight):
        return jnp.dot(normed, weight.reshape(weight.shape[0], -1), preferred_element_type=jnp.float32)
    gate = project(gate_weight).astype(jnp.bfloat16)
    conv_input = jnp.concatenate([project(value_weight), project(inflow_weight), project(readout_weight)], axis=1).astype(jnp.bfloat16)
    step = jax.nn.softplus(project(step_weight)).reshape(count, 2, SSD_HEADS)
    taps = jnp.concatenate([conv_values, conv_inflow.reshape(CONV, -1), conv_readout.reshape(CONV, -1)], axis=1).astype(jnp.float32)
    reach = CONV // 2
    padded = jnp.pad(conv_input.astype(jnp.float32), ((reach, reach), (0, 0)))
    conv_sum = padded[0:count] * taps[0]
    for tap in range(1, CONV):
        conv_sum = conv_sum + padded[tap:tap + count] * taps[tap]
    conv_out = lax.optimization_barrier(jax.nn.silu(conv_sum).astype(jnp.bfloat16)).astype(jnp.float32)
    xs = conv_out[:, :INNER].reshape(count, SSD_HEADS, HEAD_DIM)
    inflow = conv_out[:, INNER:INNER + GROUPS * STATE].reshape(count, GROUPS, STATE)
    readout = conv_out[:, INNER + GROUPS * STATE:].reshape(count, GROUPS, STATE)
    decay = -jnp.exp(log_rate) * jnp.transpose(step, (1, 0, 2))
    forward = run_blocks(xs * step[:, 0, :, None], decay[0], inflow, readout)
    backward = jnp.flip(run_blocks(jnp.flip(xs * step[:, 1, :, None], 0), jnp.flip(decay[1], 0), jnp.flip(inflow, 0), jnp.flip(readout, 0)), 0)
    combined = (forward + backward).reshape(count, INNER) * jax.nn.silu(gate.astype(jnp.float32))
    grouped = combined.reshape(count, GROUPS, -1)
    grouped = grouped * lax.rsqrt(lax.optimization_barrier(jnp.mean(grouped * grouped, axis=2, keepdims=True)) + EPS)
    state_features = (grouped.reshape(count, INNER) * group_gain.astype(jnp.float32)).astype(jnp.bfloat16)
    repeat = ATT_HEADS // KV_HEADS
    positions = jnp.arange(count, dtype=jnp.int32)
    queries = axial_rope(project(query_weight).astype(jnp.bfloat16).reshape(count, ATT_HEADS, HEAD_DIM), positions)
    keys = axial_rope(project(key_weight).astype(jnp.bfloat16).reshape(count, KV_HEADS, HEAD_DIM), positions)
    vectors = project(vector_weight).astype(jnp.bfloat16).reshape(count, KV_HEADS, HEAD_DIM)
    key_pad = jnp.pad(keys, ((WINDOW, WINDOW), (0, 0), (0, 0)))
    vector_pad = jnp.pad(vectors, ((WINDOW, WINDOW), (0, 0), (0, 0)))
    grouped_q = queries.reshape(count, KV_HEADS, repeat, HEAD_DIM)
    band = QBLOCK + 2 * WINDOW
    sinks = sink_logit.reshape(KV_HEADS, repeat, 1, 1)

    def attend(index):
        start = (index * QBLOCK).astype(jnp.int32)
        block_q = lax.dynamic_slice_in_dim(grouped_q, start, QBLOCK, 0).astype(jnp.float32)
        block_k = lax.dynamic_slice_in_dim(key_pad, start, band, 0).astype(jnp.float32)
        block_v = lax.dynamic_slice_in_dim(vector_pad, start, band, 0).astype(jnp.float32)
        scores = jnp.einsum('qkrd,skd->krqs', block_q, block_k) * HEAD_DIM ** (-0.5)
        query_pos = start + jnp.arange(QBLOCK, dtype=jnp.int32)
        key_pos = start - WINDOW + jnp.arange(band, dtype=jnp.int32)
        valid = (jnp.abs(query_pos[:, None] - key_pos[None, :]) <= WINDOW) & (key_pos >= 0)[None, :] & (key_pos < count)[None, :]
        scores = jnp.where(valid, scores, -jnp.inf)
        top = jnp.maximum(lax.optimization_barrier(jnp.max(scores, axis=-1, keepdims=True)), sinks)
        expo = jnp.exp(scores - top)
        total = lax.optimization_barrier(jnp.sum(expo, axis=-1, keepdims=True)) + jnp.exp(sinks - top)
        probs = lax.optimization_barrier(expo.astype(jnp.bfloat16)).astype(jnp.float32)
        values = jnp.einsum('krqs,skd->qkrd', probs, block_v) / jnp.transpose(total, (2, 0, 1, 3))
        logs = jnp.transpose((top + jnp.log(total))[..., 0], (2, 0, 1)).reshape(QBLOCK, -1)
        return (values.astype(jnp.bfloat16).reshape(QBLOCK, -1), logs)
    feats, logs = lax.map(attend, jnp.arange(count // QBLOCK, dtype=jnp.int32))
    window_features = feats.reshape(count, ATT_WIDTH)
    log_total = logs.reshape(count, ATT_HEADS)
    state_cols = INNER // N_TP
    window_cols = ATT_WIDTH // N_TP
    summed = jnp.zeros((count, D), jnp.float32)
    for group in range(N_TP):
        part = jnp.dot(state_features[:, group * state_cols:(group + 1) * state_cols], state_out[group * state_cols:(group + 1) * state_cols], preferred_element_type=jnp.float32)
        part = part + jnp.dot(window_features[:, group * window_cols:(group + 1) * window_cols], window_out[group * window_cols:(group + 1) * window_cols], preferred_element_type=jnp.float32)
        summed = summed + lax.optimization_barrier(part.astype(jnp.bfloat16)).astype(jnp.float32)
    return (summed.astype(jnp.bfloat16), log_total)
```

```python
import jax
import jax.numpy as jnp
from jax import lax
from jax.experimental import pallas as pl
from jax.experimental.pallas import tpu as pltpu
from jax.sharding import PartitionSpec as P


HEAD_DIM = 64
CONV = 5
SSD_BLOCK = 128
WINDOW = 128
GRID_W = 64


EPS = 1e-06
ROPE_BASE = 10000.0
HIGHEST = lax.Precision.HIGHEST
F32 = jnp.float32
BF16 = jnp.bfloat16
PAD = 16


def iota(shape, dim):
    return lax.broadcasted_iota(jnp.int32, shape, dim)


def exact(a, b):
    return jnp.dot(a, b, precision=HIGHEST, preferred_element_type=F32)


def spread(heads):
    shape = (heads, heads * HEAD_DIM)
    return (iota(shape, 1) // HEAD_DIM == iota(shape, 0)).astype(F32)


def inner_t(a, b):
    return lax.dot_general(a, b, (((1,), (1,)), ((), ())), preferred_element_type=F32)


def outer_t(a, b):
    return lax.dot_general(a, b, (((0,), (0,)), ((), ())), preferred_element_type=F32)


def summary_kernel(cells_ref, sd_ref, out_ref):
    count = cells_ref.shape[0]
    heads = sd_ref.shape[1] // 4
    wide = heads * HEAD_DIM
    state = out_ref.shape[1] - PAD
    x = cells_ref[:, :wide].astype(F32)
    writes = cells_ref[:, wide : wide + state]
    expand = spread(heads)
    row = iota((count, count), 0)
    col = iota((count, count), 1)
    for e in range(2):
        step = sd_ref[:, e * heads : (e + 1) * heads]
        decay = sd_ref[:, (2 + e) * heads : (3 + e) * heads]
        span = (col > row) if e == 0 else (col < row)
        rest = exact(span.astype(F32), decay)
        scaled = (x * exact(jnp.exp(rest) * step, expand)).astype(BF16)
        out_ref[e, :state, :] = outer_t(writes, scaled).astype(BF16)
        total = exact(jnp.broadcast_to(jnp.sum(decay, axis=0, keepdims=True), (8, heads)), expand)
        total = total[0:1]
        high = total.astype(BF16).astype(F32)
        place = iota((PAD, wide), 0)
        packed = jnp.where(place == 0, high, jnp.where(place == 1, total - high, 0.0))
        out_ref[e, state:, :] = packed.astype(BF16)


def mixer_kernel(cells_ref, sd_ref, sdt_ref, start_ref, gate_ref, gain_ref, out_ref, back_ref, carry_ref):
    blocks, _, size = sdt_ref.shape
    heads = sd_ref.shape[1] // 4
    wide = heads * HEAD_DIM
    state = start_ref.shape[1]
    expand = spread(heads)
    row = iota((size, size), 0)
    col = iota((size, size), 1)
    lower = (row >= col).astype(F32)
    upper = (row <= col).astype(F32)

    carry_ref[...] = start_ref[1]

    def backward(index, _):
        block = blocks - 1 - index
        rows = pl.ds(pl.multiple_of(block * size, size), size)
        back_ref[block] = carry_ref[...].astype(BF16)
        step = sd_ref[rows, heads : 2 * heads]
        cum = exact(upper, sd_ref[rows, 3 * heads : 4 * heads])
        edge = cum[0:1]
        x = cells_ref[rows, :wide].astype(F32)
        scaled = (x * exact(jnp.exp(edge - cum) * step, expand)).astype(BF16)
        fresh = outer_t(cells_ref[rows, wide : wide + state], scaled)
        fade = exact(jnp.broadcast_to(jnp.exp(edge), (8, heads)), expand)[0:1]
        carry_ref[...] = fade * carry_ref[...] + fresh
        return 0

    lax.fori_loop(0, blocks, backward, 0)
    carry_ref[...] = start_ref[0]

    def forward(block, _):
        rows = pl.ds(pl.multiple_of(block * size, size), size)
        cum_f = exact(lower, sd_ref[rows, 2 * heads : 3 * heads])
        cum_b = exact(upper, sd_ref[rows, 3 * heads : 4 * heads])
        flat = sdt_ref[block]
        step_ft = flat[:heads]
        step_bt = flat[heads : 2 * heads]
        cum_ft = exact(flat[2 * heads : 3 * heads], upper)
        cum_bt = exact(flat[3 * heads :], lower)
        x = cells_ref[rows, :wide]
        writes = cells_ref[rows, wide : wide + state]
        reads = cells_ref[rows, wide + state :]
        cross = inner_t(reads, writes)
        parts = []
        for h in range(heads):
            one = slice(h, h + 1)
            seg = jnp.where(
                row >= col, cum_f[:, one] - cum_ft[one], cum_b[:, one] - cum_bt[one]
            )
            scale = jnp.where(
                row > col,
                step_ft[one],
                jnp.where(row < col, step_bt[one], step_ft[one] + step_bt[one]),
            )
            weight = (cross * jnp.exp(seg) * scale).astype(BF16)
            parts.append(
                jnp.dot(
                    weight, x[:, h * HEAD_DIM : (h + 1) * HEAD_DIM], preferred_element_type=F32
                )
            )
        y = jnp.concatenate(parts, axis=1)
        y = y + exact(jnp.exp(cum_f), expand) * jnp.dot(
            reads, carry_ref[...].astype(BF16), preferred_element_type=F32
        )
        y = y + exact(jnp.exp(cum_b), expand) * jnp.dot(
            reads, back_ref[block], preferred_element_type=F32
        )
        gate = gate_ref[rows, :].astype(F32)
        y = y * (gate * jax.nn.sigmoid(gate))
        y = y * lax.rsqrt(jnp.mean(y * y, axis=1, keepdims=True) + EPS)
        out_ref[rows, :] = (y * gain_ref[...].astype(F32)).astype(BF16)
        edge = cum_f[size - 1 : size]
        step = sd_ref[rows, :heads]
        scaled = (x.astype(F32) * exact(jnp.exp(edge - cum_f) * step, expand)).astype(BF16)
        fade = exact(jnp.broadcast_to(jnp.exp(edge), (8, heads)), expand)[0:1]
        carry_ref[...] = fade * carry_ref[...] + outer_t(writes, scaled)
        return 0

    lax.fori_loop(0, blocks, forward, 0)


def attend_kernel(place_ref, sink_ref, q_ref, kv_ref, turn_ref, swap_ref, out_ref, log_ref, keys_ref):
    count = q_ref.shape[0]
    q_count = q_ref.shape[1] // HEAD_DIM
    kv_width = kv_ref.shape[1] // 2
    repeat = q_count * HEAD_DIM // kv_width
    size = SSD_BLOCK
    band = size + 2 * WINDOW
    swap = swap_ref[...]

    def turned(part, rows):
        swapped = jnp.dot(part, swap, preferred_element_type=F32)
        table = turn_ref[rows, :]
        return (part.astype(F32) * table[:, :HEAD_DIM] + swapped * table[:, HEAD_DIM:]).astype(BF16)

    def prepare(block, _):
        rows = pl.ds(pl.multiple_of(block * size, size), size)
        for g in range(kv_width // HEAD_DIM):
            keys_ref[g, rows, :] = turned(
                kv_ref[rows, g * HEAD_DIM : (g + 1) * HEAD_DIM], rows
            )
        return 0

    lax.fori_loop(0, kv_ref.shape[0] // size, prepare, 0)
    row = iota((size, band), 0)
    col = iota((size, band), 1)
    near = (col >= row) & (col - row <= 2 * WINDOW)
    lane = iota((size, q_count), 1)

    def one(block, _):
        start = pl.multiple_of(block * size, size)
        rows = pl.ds(start, size)
        reach = pl.ds(start, band)
        key_pos = place_ref[0] + start - WINDOW + col
        valid = near & (key_pos >= 0) & (key_pos < place_ref[1])
        logs = jnp.zeros((size, q_count), F32)
        outs = []
        for h in range(q_count):
            g = h // repeat
            query = turned(
                q_ref[rows, h * HEAD_DIM : (h + 1) * HEAD_DIM], pl.ds(start + WINDOW, size)
            )
            scores = inner_t(query, keys_ref[g, reach, :]) * HEAD_DIM ** (-0.5)
            scores = jnp.where(valid, scores, -jnp.inf)
            sink = sink_ref[h]
            top = jnp.maximum(jnp.max(scores, axis=1, keepdims=True), sink)
            expo = jnp.exp(scores - top)
            total = jnp.sum(expo, axis=1, keepdims=True) + jnp.exp(sink - top)
            first = kv_width + g * HEAD_DIM
            values = jnp.dot(
                expo.astype(BF16),
                kv_ref[reach, first : first + HEAD_DIM],
                preferred_element_type=F32,
            )
            outs.append((values / total).astype(BF16))
            logs = jnp.where(lane == h, top + jnp.log(total), logs)
        out_ref[rows, :] = jnp.concatenate(outs, axis=1)
        log_ref[rows, :] = logs
        return 0

    lax.fori_loop(0, count // size, one, 0)


def call(kernel, out_shape, args, scratch=(), scalars=0, flops=10**8):
    vmem = pl.BlockSpec(memory_space=pltpu.VMEM)
    smem = pl.BlockSpec(memory_space=pltpu.SMEM)
    return pl.pallas_call(
        kernel,
        out_shape=out_shape,
        in_specs=[smem] * scalars + [vmem] * (len(args) - scalars),
        out_specs=jax.tree.map(lambda _: vmem, out_shape),
        scratch_shapes=list(scratch),
        cost_estimate=pl.CostEstimate(flops=flops, bytes_accessed=4 * 10**6, transcendentals=0),
        compiler_params=pltpu.CompilerParams(vmem_limit_bytes=40 * 2**20),
    )(*args)


def with_halo(cells, sides, width):
    for axis, dim in sides:
        count = lax.axis_size(axis)
        ends = count - 1
        head = lax.slice_in_dim(cells, 0, width, axis=dim)
        tail = lax.slice_in_dim(cells, cells.shape[dim] - width, cells.shape[dim], axis=dim)
        cells = jnp.concatenate(
            [
                lax.ppermute(tail, axis, [(i, (i + 1) % count) for i in range(ends)]),
                cells,
                lax.ppermute(head, axis, [((i + 1) % count, i) for i in range(ends)]),
            ],
            axis=dim,
        )
    return cells


def flatten_rows(weight):
    return weight.reshape(weight.shape[0], -1)


def shards(
    tokens,
    input_gain,
    gate_weight,
    value_weight,
    inflow_weight,
    readout_weight,
    step_weight,
    conv_values,
    conv_inflow,
    conv_readout,
    log_rate,
    group_gain,
    query_weight,
    key_weight,
    vector_weight,
    sink_logit,
    state_out,
    window_out,
):
    count = tokens.shape[0]
    offset = lax.axis_index("sp") * count
    seq_total = count * lax.axis_size("sp")
    heads = step_weight.shape[2]
    groups = inflow_weight.shape[1]
    state_len = inflow_weight.shape[2]
    inner_local = value_weight.shape[1]
    q_count = query_weight.shape[1] // HEAD_DIM
    kv_count = key_weight.shape[1] // HEAD_DIM
    kv_width = key_weight.shape[1]
    wide = tokens.astype(F32)
    normed = (
        wide
        * lax.rsqrt(jnp.mean(wide * wide, axis=1, keepdims=True) + EPS)
        * input_gain.astype(F32)
    ).astype(BF16)

    def whole(parts):
        return lax.all_gather(jnp.concatenate(parts, axis=1), "sp", axis=0, tiled=True)

    own = (flatten_rows(inflow_weight), flatten_rows(readout_weight), flatten_rows(step_weight))
    first_matrix = whole((value_weight,) + own)
    rest_matrix = whole((key_weight, vector_weight, gate_weight, query_weight))
    first = jnp.dot(normed, first_matrix, preferred_element_type=F32)
    rest = jnp.dot(normed, rest_matrix, preferred_element_type=F32).astype(BF16)
    conv_width = inner_local + 2 * groups * state_len
    conv_input = first[:, :conv_width].astype(BF16)
    step = jax.nn.softplus(first[:, conv_width:])
    keyvals = rest[:, : 2 * kv_width]
    gate = rest[:, 2 * kv_width : 2 * kv_width + inner_local]
    queries = rest[:, 2 * kv_width + inner_local :]

    reach_rows = CONV // 2
    padded = with_halo(conv_input, (("sp", 0),), CONV // 2).astype(F32)
    taps = jnp.concatenate(
        [conv_values, flatten_rows(conv_inflow), flatten_rows(conv_readout)], axis=1
    ).astype(F32)
    conv_sum = padded[0:count] * taps[0]
    for tap in range(1, 2 * reach_rows + 1):
        conv_sum = conv_sum + padded[tap : tap + count] * taps[tap]
    cells = jax.nn.silu(conv_sum).astype(BF16)
    rates = jnp.transpose(log_rate, (1, 0, 2)).reshape(count, 2 * heads)
    sd = jnp.concatenate([step, -jnp.exp(rates) * step], axis=1)
    blocks = count // SSD_BLOCK
    sdt = jnp.transpose(sd.reshape(blocks, SSD_BLOCK, 4 * heads), (0, 2, 1))

    summary = call(
        summary_kernel,
        jax.ShapeDtypeStruct((2, state_len + PAD, inner_local), BF16),
        (cells, sd),
    )
    everyone = lax.all_gather(summary, "sp")
    out_stack, everyone = lax.optimization_barrier(
        (jnp.concatenate([state_out, window_out], axis=0), everyone)
    )
    out_matrix = lax.all_gather(out_stack, "sp", axis=1, tiled=True)
    seats = lax.axis_size("sp")
    place = lax.axis_index("sp")
    totals = everyone[:, :, state_len].astype(F32) + everyone[:, :, state_len + 1].astype(F32)
    seat = jnp.arange(seats)
    starts = []
    for e in range(2):
        ahead = seat < place if e == 0 else seat > place
        between = (seat[None, :] > seat[:, None]) if e == 0 else (seat[None, :] < seat[:, None])
        between = (between & ahead[None, :])[:, :, None]
        fade = jnp.sum(jnp.where(between, totals[None, :, e], 0.0), axis=1)
        fade = jnp.where(ahead[:, None], jnp.exp(fade), 0.0)
        starts.append(jnp.sum(fade[:, None, :] * everyone[:, e, :state_len].astype(F32), axis=0))
    starts = jnp.stack(starts)
    state_features = call(
        mixer_kernel,
        jax.ShapeDtypeStruct((count, inner_local), BF16),
        (cells, sd, sdt, starts, gate, group_gain[None]),
        (
            pltpu.VMEM((blocks, state_len, inner_local), BF16),
            pltpu.VMEM((state_len, inner_local), F32),
        ),
        flops=10**10,
    )

    beside = with_halo(keyvals, (("sp", 0),), WINDOW)
    quarter = HEAD_DIM // 4
    freqs = ROPE_BASE ** (-jnp.arange(quarter).astype(F32) / quarter)
    spots = offset - WINDOW + jnp.arange(count + 2 * WINDOW, dtype=jnp.int32)
    row_angle = (spots // GRID_W).astype(F32)[:, None] * freqs
    col_angle = (spots % GRID_W).astype(F32)[:, None] * freqs
    angles = jnp.concatenate([row_angle, col_angle], axis=1)
    cosine = jnp.cos(angles)
    sine = jnp.sin(angles)

    def doubled(table, sign):
        low = table[:, :quarter]
        high = table[:, quarter:]
        return [sign * low, low, sign * high, high]

    turn = jnp.concatenate(doubled(cosine, 1.0) + doubled(sine, -1.0), axis=1)
    channel = jnp.arange(HEAD_DIM)
    partner = channel + jnp.where(channel % (2 * quarter) < quarter, quarter, -quarter)
    swap = (channel[:, None] == partner[None, :]).astype(BF16)
    limits = jnp.stack([offset, seq_total]).astype(jnp.int32)
    window_features, log_total = call(
        attend_kernel,
        (
            jax.ShapeDtypeStruct((count, q_count * HEAD_DIM), BF16),
            jax.ShapeDtypeStruct((count, q_count), F32),
        ),
        (limits, sink_logit, queries, beside, turn, swap),
        (pltpu.VMEM((kv_count, count + 2 * WINDOW, HEAD_DIM), BF16),),
        scalars=2,
        flops=10**10,
    )
    features = jnp.concatenate([state_features, window_features], axis=1)
    terms = jnp.dot(features, out_matrix, preferred_element_type=F32)
    mixed = lax.psum_scatter(terms.astype(BF16), "tp", scatter_dimension=1, tiled=True)
    return (mixed, log_total)


def solution(mesh):
    placed = (
        P("sp", None),
        P(),
        P("sp", "tp"),
        P("sp", "tp"),
        P("sp", "tp", None),
        P("sp", "tp", None),
        P("sp", None, "tp"),
        P(None, "tp"),
        P(None, "tp", None),
        P(None, "tp", None),
        P(None, "sp", "tp"),
        P("tp"),
        P("sp", "tp"),
        P("sp", "tp"),
        P("sp", "tp"),
        P("tp"),
        P("tp", "sp"),
        P("tp", "sp"),
    )
    return jax.shard_map(
        shards,
        mesh=mesh,
        in_specs=placed,
        out_specs=(P("sp", "tp"), P("sp", "tp")),
        check_vma=False,
    )
```
